256 devices in a mesh: grp: 2 (over z), kv: 16 (over y, core), tp: 8 (over x).
Axes of the slice: x: 8, y: 8, z: 2, core: 2. Of those that a mesh axis runs over, the one named last changes fastest.
The devices are a block of a 8x8x16 slice.
Arguments:
- tokens: bfloat16 [256, 4096], P('grp', ('kv', 'tp')), parts along dimension 0, may hold values from -12 to 12
- gain_in: bfloat16 [4096], P(('kv', 'tp')), may hold values from 0.099609375 to 1.8984375
- gate_in: bfloat16 [4096, 11008], P('kv', 'tp'), may hold values from -0.09375 to 0.09375
- up_in: bfloat16 [4096, 11008], P('kv', 'tp'), may hold values from -0.09375 to 0.09375
- down_in: bfloat16 [11008, 4096], P('tp', 'kv'), may hold values from -0.21875 to 0.21875
- gain_mix: bfloat16 [4096], P(('kv', 'tp')), may hold values from 0.099609375 to 1.8984375
- w_query: bfloat16 [4096, 1024], P('kv', 'tp'), may hold values from -0.09375 to 0.09375
- w_key: bfloat16 [4096, 1024], P('kv', 'tp'), may hold values from -0.09375 to 0.09375
- w_value: bfloat16 [4096, 2048], P('kv', 'tp'), may hold values from -0.09375 to 0.09375
- w_gate: bfloat16 [4096, 2048], P('kv', 'tp'), may hold values from -0.09375 to 0.09375
- w_mixout: bfloat16 [2048, 4096], P('tp', 'kv'), may hold values from -0.125 to 0.125
- forget_rate: float32 [8], P('tp'), may hold values from 0.01 to 0.7
- state_in: float32 [256, 8, 128, 256], P(('grp', 'kv'), 'tp'), parts along dimension 0, may hold values from -0.6 to 0.6
- positions: int32 [256], P(('grp', 'kv')), parts along dimension 0, may hold values from 0 to 8191
- gain_out: bfloat16 [4096], P(('kv', 'tp')), may hold values from 0.099609375 to 1.8984375
- gate_out: bfloat16 [4096, 11008], P('kv', 'tp'), may hold values from -0.09375 to 0.09375
- up_out: bfloat16 [4096, 11008], P('kv', 'tp'), may hold values from -0.09375 to 0.09375
- down_out: bfloat16 [11008, 4096], P('tp', 'kv'), may hold values from -0.21875 to 0.21875
Outputs:
- result: bfloat16 [256, 4096], P('grp', ('kv', 'tp')), parts along dimension 0
- new_state: float32 [256, 8, 128, 256], P(('grp', 'kv'), 'tp'), parts along dimension 0
The draws below stay inside these ranges and needn't reach their ends.
There are 2 independent parts, one for each index of `grp`. The reference program is written for one: setup_inputs(seed, part) draws one part's arguments, and reference() takes and returns one part's arrays. A program takes and returns all parts, laid end to end along the dimension named above; an argument that names none is the same for every part. Nothing has to cross between parts.
All inputs are finite; a program needn't handle non-finite values.
Results may differ from the reference program's by a relative error of at most 0.024.
Values may be sent and summed in bfloat16 or wider, within the bound.
A program may use at most 64 MiB of HBM per device.

```python
import math
import jax
import jax.numpy as jnp
from jax import lax

D = 4096
FF = 11008
HEADS = 8
DK = 128
DV = 256
B = 128
HEAD_GROUP = 1
UNIT_GROUP = 1376
N_TP = 8


def draw_tokens(key, part):
    column_scale = jnp.exp(jnp.log(4.0) * jnp.arange(D, dtype=jnp.float32) / D)
    base = jnp.clip(jax.random.normal(jax.random.fold_in(key, 11), (B, D), jnp.float32), -3.0, 3.0)
    return (base * column_scale[None, :]).astype(jnp.bfloat16)


def plant(values, key, low, largest):
    spot = [jax.random.randint(jax.random.fold_in(key, axis), (), 0, length) for axis, length in enumerate(values.shape)]
    longest = values.shape.index(max(values.shape))
    next_to = spot[:longest] + [(spot[longest] + 1) % values.shape[longest]] + spot[longest + 1:]
    return values.at[tuple(spot)].set(low).at[tuple(next_to)].set(largest)


def with_spikes(entries, rng, source, target, blocks, factor):
    def block_of(axis_at):
        return (jnp.arange(entries.shape[axis_at]) // (entries.shape[axis_at] // blocks)).reshape((-1,) + (1,) * (entries.ndim - 1 - axis_at))

    near = jax.random.permutation(rng, blocks)[block_of(target)]
    far = (block_of(target) + blocks // 2) % blocks
    return jnp.where((block_of(source) == near) | (block_of(source) == far), factor * entries, entries)


def levels(own_key, shape, pieces, low, top_value):
    level = 1.0
    for axis_at, blocks in pieces:
        steps = jax.random.uniform(jax.random.fold_in(jax.random.fold_in(own_key, 6), axis_at), (blocks,), jnp.float32, low / len(pieces), top_value / len(pieces))
        level = level * jnp.repeat(jnp.exp(steps), shape[axis_at] // blocks).reshape((-1,) + (1,) * (len(shape) - 1 - axis_at))
    return level


def noise(key, extent, deviation, most, shards=(), kind=jnp.bfloat16):
    level = levels(key, extent, shards, -0.22, 0.18) if shards else 1.0
    array = jax.random.normal(key, extent, jnp.float32) * deviation * level
    return jnp.minimum(jnp.maximum(array, -most), most).astype(kind)


def heavy_noise(key, shape, scale, bound, cuts, heavy, kind=jnp.bfloat16):
    drawn = scale * jax.random.normal(key, shape, jnp.float32)
    if cuts:
        drawn = drawn * levels(key, shape, cuts, -0.22, 0.18)
    return jnp.clip(with_spikes(drawn, jax.random.fold_in(key, 3), *heavy), -bound, bound).astype(kind)


def setup_inputs(seed: int = 0, part: int = 0) -> dict:
    streams_of = jax.random.split(jax.random.key(seed), 19)
    part_splits = jax.random.split(jax.random.fold_in(streams_of[18], part), 19)
    tokens = draw_tokens(jax.random.fold_in(jax.random.fold_in(streams_of[18], part), 71), part)
    gain_in = jnp.clip(1.0 + 0.18 * jax.random.normal(streams_of[1], (D,), jnp.float32), 0.099609375, 1.8984375).astype(jnp.bfloat16)
    gate_in = noise(streams_of[2], (D, FF), D ** -0.5, 0.09375, ((0, 16), (1, 8)))
    up_in = noise(streams_of[3], (D, FF), D ** -0.5, 0.09375, ((0, 16), (1, 8)))
    down_in = heavy_noise(streams_of[4], (FF, D), (FF // 8) ** -0.5, 0.21875, ((0, 8), (1, 16)), (0, 1, 16, 2.0))
    gain_mix = jnp.clip(1.0 + 0.18 * jax.random.normal(streams_of[5], (D,), jnp.float32), 0.099609375, 1.8984375).astype(jnp.bfloat16)
    w_query = noise(streams_of[6], (D, HEADS * DK), D ** -0.5, 0.09375, ((0, 16), (1, 8)))
    w_key = noise(streams_of[7], (D, HEADS * DK), D ** -0.5, 0.09375, ((0, 16), (1, 8)))
    w_value = noise(streams_of[8], (D, HEADS * DV), D ** -0.5, 0.09375, ((0, 16), (1, 8)))
    w_gate = noise(streams_of[9], (D, HEADS * DV), D ** -0.5, 0.09375, ((0, 16), (1, 8)))
    w_mixout = noise(streams_of[10], (HEADS * DV, D), (HEADS * DV) ** -0.5, 0.125, ((0, 8), (1, 16)))
    forget_rate = jnp.clip(jnp.exp(math.log(0.7) - 4.248495 * jax.random.uniform(streams_of[11], (HEADS,), jnp.float32) ** levels(streams_of[11], (HEADS,), ((0, 8),), -0.2, 0.2)), 0.01, 0.7)
    state_in = noise(part_splits[12], (B, HEADS, DK, DV), 0.1, 0.6, ((0, 16), (1, 8)), jnp.float32)
    positions = plant(jax.random.randint(part_splits[13], (B,), 0, 8192), jax.random.fold_in(part_splits[13], 1), 0, 8191).astype(jnp.int32)
    gain_out = jnp.clip(1.0 + 0.18 * jax.random.normal(streams_of[14], (D,), jnp.float32), 0.099609375, 1.8984375).astype(jnp.bfloat16)
    gate_out = noise(streams_of[15], (D, FF), D ** -0.5, 0.09375, ((0, 16), (1, 8)))
    up_out = noise(streams_of[16], (D, FF), D ** -0.5, 0.09375, ((0, 16), (1, 8)))
    down_out = heavy_noise(streams_of[17], (FF, D), (FF // 8) ** -0.5, 0.21875, ((0, 8), (1, 16)), (0, 1, 16, 2.0))
    return dict(tokens=tokens, gain_in=gain_in, gate_in=gate_in, up_in=up_in, down_in=down_in, gain_mix=gain_mix, w_query=w_query, w_key=w_key, w_value=w_value, w_gate=w_gate, w_mixout=w_mixout, forget_rate=forget_rate, state_in=state_in, positions=positions, gain_out=gain_out, gate_out=gate_out, up_out=up_out, down_out=down_out)


epsilon = 1e-06

def group_sum(hidden, w_down):
    grouped = hidden.reshape(B, N_TP, UNIT_GROUP).astype(jnp.float32)
    weights = w_down.reshape(N_TP, UNIT_GROUP, D).astype(jnp.float32)
    partials = jnp.einsum('bgc,gcd->gbd', grouped, weights)
    rounded = lax.optimization_barrier(partials.astype(jnp.bfloat16)).astype(jnp.float32)
    return lax.optimization_barrier(jnp.sum(rounded, axis=0))

def half_mlp(tokens, gain_row, w_gate, w_up, w_down):
    widened = tokens.astype(jnp.float32)
    factor = lax.rsqrt(lax.optimization_barrier(jnp.mean(widened * widened, axis=-1, keepdims=True)) + epsilon)
    normed = (widened * gain_row.astype(jnp.float32)).astype(jnp.bfloat16)
    gate_sum = factor * jnp.dot(normed, w_gate, preferred_element_type=jnp.float32)
    up_sum = factor * jnp.dot(normed, w_up, preferred_element_type=jnp.float32)
    hidden = (jax.nn.silu(gate_sum) * up_sum).astype(jnp.bfloat16)
    lowered = group_sum(hidden, w_down)
    return (widened + 0.5 * lowered).astype(jnp.bfloat16)

def rotate(vectors, positions):
    half_dim = vectors.shape[-1] // 2
    inverse = jnp.power(10000.0, -jnp.arange(half_dim, dtype=jnp.float32) * 2.0 / vectors.shape[-1])
    angles = positions.astype(jnp.float32)[:, None] * inverse[None, :]
    cosine = jnp.cos(angles)[:, None, :]
    sine_part = jnp.sin(angles)[:, None, :]
    first_half = vectors[..., :half_dim]
    second_half = vectors[..., half_dim:]
    return jnp.concatenate([first_half * cosine - second_half * sine_part, first_half * sine_part + second_half * cosine], axis=-1)

def retention_step(normed, factor, w_query, w_key, w_value, w_gate, forget_rate, state_in, positions):
    count_rows = normed.shape[0]

    def project(weight, head_dim):
        product = factor * jnp.dot(normed, weight, preferred_element_type=jnp.float32)
        rounded = lax.optimization_barrier(product.astype(jnp.bfloat16))
        return rounded.astype(jnp.float32).reshape(count_rows, HEADS, head_dim)
    queries = rotate(project(w_query, DK), positions)
    key_rot = rotate(project(w_key, DK), positions) * DK ** (-0.5)
    values_now = project(w_value, DV)
    gates_now = project(w_gate, DV)
    decays = jnp.exp(-forget_rate)
    carried = jnp.einsum('bhd,bhde->bhe', queries, state_in, precision=lax.Precision.HIGHEST)
    present = lax.optimization_barrier(jnp.sum(queries * key_rot, axis=-1, keepdims=True)) * values_now
    retained = present + decays[None, :, None] * carried
    new_state = decays[None, :, None, None] * state_in + key_rot[..., None] * values_now[..., None, :]
    normed_heads = retained * lax.rsqrt(lax.optimization_barrier(jnp.mean(retained * retained, axis=-1, keepdims=True)) + epsilon)
    mixed = (jax.nn.silu(gates_now) * normed_heads).astype(jnp.bfloat16)
    return (mixed.reshape(count_rows, HEADS * DV), new_state)

def reference(tokens, gain_in, gate_in, up_in, down_in, gain_mix, w_query, w_key, w_value, w_gate, w_mixout, forget_rate, state_in, positions, gain_out, gate_out, up_out, down_out):
    after_first = half_mlp(tokens, gain_in, gate_in, up_in, down_in)
    widened = after_first.astype(jnp.float32)
    factor = lax.rsqrt(lax.optimization_barrier(jnp.mean(widened * widened, axis=-1, keepdims=True)) + epsilon)
    normed = (widened * gain_mix.astype(jnp.float32)).astype(jnp.bfloat16)
    mixed, new_state = retention_step(normed, factor, w_query, w_key, w_value, w_gate, forget_rate, state_in, positions)
    grouped = mixed.reshape(B, N_TP, HEAD_GROUP * DV).astype(jnp.float32)
    weights = w_mixout.reshape(N_TP, HEAD_GROUP * DV, D).astype(jnp.float32)
    partials = jnp.einsum('bgc,gcd->gbd', grouped, weights)
    rounded = lax.optimization_barrier(partials.astype(jnp.bfloat16)).astype(jnp.float32)
    second = (widened + lax.optimization_barrier(jnp.sum(rounded, axis=0))).astype(jnp.bfloat16)
    result = half_mlp(second, gain_out, gate_out, up_out, down_out)
    return (result, new_state)
```

```python
import functools
import math

import jax
import jax.numpy as jnp
from jax import lax
from jax.experimental import pallas as pl
from jax.experimental.pallas import tpu as pltpu
from jax.sharding import PartitionSpec as P

EPS = 1e-06
BASE = 10000.0
MESH = pl.DeviceIdType.MESH
F32 = jnp.float32
BF16 = jnp.bfloat16


def far_first(n):
    return sorted(range(1, n), key=lambda j: -min(j, n - j))


def near_first(n):
    return sorted(range(1, n), key=lambda j: min(j, n - j))


def widths(total, cut):
    edges = [0, *[c for c in cut if c < total], total]
    return list(zip(edges[:-1], edges[1:]))


def tiles(first, last, step=256):
    return [(at, min(at + step, last)) for at in range(first, last, step)]


def kernel(dims, tokens, gain_in, gain_mix, gain_out, forget, positions,
           gate_in, up_in, down_in, w_query, w_key, w_value, w_gate, w_mix, state,
           gate_out, up_out, down_out,
           result, key_out, value_out, *scratch):
    NT, NY, NK, R, OWN, C, c, FF, DK, DV, D, mlp_pieces, qkv_pieces = dims
    (tok_v, gains_v, gi_v, ui_v, di_v, wq_v, wk_v, wv_v, wg_v, wm_v, st_v, go_v, uo_v, do_v, load_sem,
     xall, ss_src, ssx, ss_k, ss_b, ss_c, ssy, fac,
     part_m, sib_m, red_m, recv_m, part_q, sib_q, red_q, recv_q,
     hall, mall, px, rx, oT,
     ax_s, axs_s, sib_s, ssb_s, y_s, ssy_s, ag_s, agf_s, rx_s,
     ax_r, axs_r, sib_r, ssb_r, y_r, ssy_r, ag_r, agf_r, rx_r) = scratch

    t = lax.axis_index("tp")
    k = lax.axis_index("kv")
    core = lax.rem(k, 2)
    y = lax.div(k, 2)
    sibling = {"kv": k + 1 - 2 * core}

    def at_t(j):
        return lax.rem(t + j, NT)

    def at_y(j):
        return lax.rem(y + j, NY)

    def chip(j):
        return {"kv": 2 * at_y(j) + core}

    loads = []
    pairs = [(tokens, tok_v), (gain_in, gains_v.at[0]), (gain_mix, gains_v.at[1]), (gain_out, gains_v.at[2]),
             (gate_in, gi_v), (up_in, ui_v), (w_query, wq_v), (w_key, wk_v), (w_value, wv_v), (w_gate, wg_v),
             (down_in, di_v), (w_mix, wm_v), (state, st_v), (gate_out, go_v), (up_out, uo_v), (down_out, do_v)]
    for i, (src, dst) in enumerate(pairs):
        copy = pltpu.make_async_copy(src, dst, load_sem.at[i])
        copy.start()
        loads.append(copy)

    barrier = pltpu.get_barrier_semaphore()
    pl.semaphore_signal(barrier, inc=1, device_id=sibling, device_id_type=MESH)
    for j in far_first(NT):
        pl.semaphore_signal(barrier, inc=1, device_id={"tp": at_t(j)}, device_id_type=MESH)
    for j in far_first(NY):
        pl.semaphore_signal(barrier, inc=1, device_id=chip(j), device_id_type=MESH)

    for i in range(4):
        loads[i].wait()
    tok = tok_v[...].astype(F32)

    def column(i):
        row = jnp.broadcast_to(gains_v[i].astype(F32), (R, c))
        return row.T

    resid = tok.T
    pl.semaphore_wait(barrier, 1 + (NT - 1) + (NY - 1))

    pending = {}

    def remote(src, dst, ssem, rsem, device):
        return pltpu.make_async_remote_copy(src_ref=src, dst_ref=dst, send_sem=ssem, recv_sem=rsem,
                                            device_id=device, device_id_type=MESH)

    def flush(kind):
        for copy in pending.pop(kind, []):
            copy.wait_send()

    def gather_x(s, normed, squares):
        flush("ax")
        xall[s, t] = normed
        ss_src[s] = squares
        copies, small = [], []
        for j in far_first(NT):
            copy = remote(xall.at[s, t], xall.at[s, t], ax_s.at[j], ax_r.at[s, NT - j], {"tp": at_t(j)})
            copy.start()
            copies.append(copy)
        for j in far_first(NT):
            copy = remote(ss_src.at[s], ssx.at[s, NT - j], axs_s.at[j], axs_r.at[s, NT - j], {"tp": at_t(j)})
            copy.start()
            small.append(copy)
        for j in near_first(NT):
            remote(xall.at[s, t], xall.at[s, t], ax_s.at[j], ax_r.at[s, j], {"tp": at_t(j)}).wait_recv()
        pending["ax"] = copies + small
        whole = xall[s].astype(F32).reshape(C, R)
        return whole.T.astype(BF16)

    def squares_of_block(s, own):
        total = own
        for j in near_first(NT):
            remote(ss_src.at[s], ssx.at[s, j], axs_s.at[j], axs_r.at[s, j], {"tp": at_t(j)}).wait_recv()
            total = total + ssx[s, j]
        return total

    def scatter_y(s, pieces, compute, part, sib, red, recv, own_squares, first_piece):
        flush("y")
        copies = []
        for p in range(len(pieces)):
            compute(p)
            copy = remote(part[p].at[1 - core], sib[p], sib_s.at[p], sib_r.at[s, p], sibling)
            copy.start()
            copies.append(copy)
        block = squares_of_block(s, own_squares)
        ss_k[s] = block
        copy = remote(ss_k.at[s], ss_b.at[s], ssb_s.at[0], ssb_r.at[s], sibling)
        copy.start()
        copies.append(copy)
        for p in range(len(pieces)):
            remote(part[p].at[1 - core], sib[p], sib_s.at[p], sib_r.at[s, p], sibling).wait_recv()
            late = None
            for j in far_first(NY) + [0]:
                yd = at_y(j)
                red[p][yd] = (part[p][core, yd].astype(F32) + sib[p][yd].astype(F32)).astype(BF16)
                if late is not None:
                    late.start()
                    copies.append(late)
                late = None
                if j:
                    late = remote(red[p].at[yd], recv[p].at[NY - j], y_s.at[p, j], y_r.at[s, p, NY - j], chip(j))
        remote(ss_k.at[s], ss_b.at[s], ssb_s.at[0], ssb_r.at[s], sibling).wait_recv()
        chip_sum = block + ss_b[s]
        ss_c[s] = chip_sum
        for j in far_first(NY):
            copy = remote(ss_c.at[s], ssy.at[s, NY - j], ssy_s.at[j], ssy_r.at[s, NY - j], chip(j))
            copy.start()
            copies.append(copy)
        pending["y"] = copies
        total = chip_sum
        for j in near_first(NY):
            remote(ss_c.at[s], ssy.at[s, j], ssy_s.at[j], ssy_r.at[s, j], chip(j)).wait_recv()
            total = total + ssy[s, j]
        wide = jnp.broadcast_to(total, (128, R)).T
        fac[s] = lax.rsqrt(wide / D + EPS)
        factor = fac[s, pl.ds(pl.multiple_of(k * OWN, OWN), OWN), :][:, :1]
        sums = []
        for p in range(len(pieces)):
            acc = red[p][y].astype(F32)
            for j in near_first(NY):
                remote(red[p].at[y], recv[p].at[j], y_s.at[p, j], y_r.at[s, p, j], chip(j)).wait_recv()
                acc = acc + recv[p][j].astype(F32)
            sums.append(acc)
        return sums, factor

    def gather_y(s, buf):
        flush("ag")
        copies = []
        copy = remote(buf.at[k], buf.at[k], agf_s.at[0], agf_r.at[s, 0], sibling)
        copy.start()
        copies.append(copy)
        for j in far_first(NY):
            copy = remote(buf.at[k], buf.at[k], ag_s.at[j], ag_r.at[s, NY - j], chip(j))
            copy.start()
            copies.append(copy)
        for j in near_first(NY):
            slot = 2 * at_y(j) + core
            remote(buf.at[slot], buf.at[slot], ag_s.at[j], ag_r.at[s, j], chip(j)).wait_recv()
            copy = remote(buf.at[slot], buf.at[slot], agf_s.at[j], agf_r.at[s, j], sibling)
            copy.start()
            copies.append(copy)
        for j in [0] + near_first(NY):
            slot = 2 * at_y(j) + 1 - core
            remote(buf.at[slot], buf.at[slot], agf_s.at[j], agf_r.at[s, j], sibling).wait_recv()
        pending["ag"] = copies

    def scatter_x(s, product):
        flush("rx")
        px[s] = product.T.reshape(NT, c, R).astype(BF16)
        copies = []
        for j in far_first(NT):
            copy = remote(px.at[s, at_t(j)], rx.at[s, NT - j], rx_s.at[j], rx_r.at[s, NT - j], {"tp": at_t(j)})
            copy.start()
            copies.append(copy)
        pending["rx"] = copies
        total = px[s, t].astype(F32)
        for j in near_first(NT):
            remote(px.at[s, at_t(j)], rx.at[s, j], rx_s.at[j], rx_r.at[s, j], {"tp": at_t(j)}).wait_recv()
            total = total + rx[s, j].astype(F32)
        return total

    def half_mlp(s, resid, gain, gate, up, down, waits):
        squares = jnp.sum(resid * resid, axis=0, keepdims=True)
        normed = gather_x(s, (resid * gain).astype(BF16), squares)
        for i in waits[:2]:
            loads[i].wait()

        def compute(p):
            first, last = mlp_pieces[p]
            for lo, hi in tiles(first, last):
                g = jnp.dot(normed, gate[:, lo:hi], preferred_element_type=F32)
                u = jnp.dot(normed, up[:, lo:hi], preferred_element_type=F32)
                for kk in range(NK):
                    rows = slice(OWN * kk, OWN * kk + OWN)
                    part_m[p][kk % 2, kk // 2, :, lo - first:hi - first] = jnp.concatenate(
                        [g[rows], u[rows]], axis=0).astype(BF16)

        sums, factor = scatter_y(s, mlp_pieces, compute, part_m, sib_m, red_m, [r.at[s // 2] for r in recv_m],
                                 squares, 0)
        for (first, last), acc in zip(mlp_pieces, sums):
            g = factor * acc[:OWN]
            u = factor * acc[OWN:]
            hall[s // 2, k, :, first:last] = (g / (1.0 + jnp.exp(-g)) * u).astype(BF16)
        gather_y(s, hall.at[s // 2])
        loads[waits[2]].wait()
        hidden = hall[s // 2].astype(F32).reshape(R, FF).astype(BF16)
        product = jnp.dot(hidden, down[...], preferred_element_type=F32)
        return resid + 0.5 * scatter_x(s, product)

    resid = half_mlp(0, resid, column(0), gi_v, ui_v, di_v, (4, 5, 10)).astype(BF16).astype(F32)

    squares = jnp.sum(resid * resid, axis=0, keepdims=True)
    normed = gather_x(1, (resid * column(1)).astype(BF16), squares)
    for i in (6, 7, 8, 9):
        loads[i].wait()

    def compute_qkv(p):
        q = jnp.dot(normed, wq_v[...], preferred_element_type=F32)
        kk_ = jnp.dot(normed, wk_v[...], preferred_element_type=F32)
        v = jnp.dot(normed, wv_v[...], preferred_element_type=F32)
        g = jnp.dot(normed, wg_v[...], preferred_element_type=F32)
        half = DV // 2
        top = [q, kk_, v[:, :half]]
        low = [v[:, half:], g[:, :half], g[:, half:]]
        for i in range(3):
            for kk in range(NK):
                rows = slice(OWN * kk, OWN * kk + OWN)
                part_q[0][kk % 2, kk // 2, :, DK * i:DK * i + DK] = jnp.concatenate(
                    [top[i][rows], low[i][rows]], axis=0).astype(BF16)

    sums, factor = scatter_y(1, qkv_pieces, compute_qkv, part_q, sib_q, red_q, recv_q, squares, 0)
    acc = (jnp.concatenate([factor, factor], axis=0) * sums[0]).astype(BF16).astype(F32)
    q, key = acc[:OWN, :DK], acc[:OWN, DK:2 * DK]
    value = jnp.concatenate([acc[:OWN, 2 * DK:], acc[OWN:, :DK]], axis=1)
    out_gate = acc[OWN:, DK:]

    row = lax.broadcasted_iota(jnp.int32, (OWN, DK), 0)
    lane = lax.broadcasted_iota(jnp.int32, (OWN, DK), 1)
    place = jnp.zeros((OWN, DK), F32)
    for r in range(OWN):
        place = jnp.where(row == r, positions[r].astype(F32), place)
    half = DK // 2
    pair = jnp.where(lane < half, lane, lane - half).astype(F32)
    angle = place * jnp.exp(pair * (-2.0 * math.log(BASE) / DK))
    cosine = jnp.cos(angle)
    sine = jnp.where(lane < half, -jnp.sin(angle), jnp.sin(angle))

    def rotate(v):
        return v * cosine + jnp.concatenate([v[:, half:], v[:, :half]], axis=1) * sine

    q = rotate(q)
    key = rotate(key) * DK ** (-0.5)
    decay = jnp.exp(jnp.broadcast_to(-forget[0], (1, DV)))
    q_col = q.T
    loads[12].wait()
    carried = jnp.concatenate(
        [jnp.sum(st_v[b] * q_col[:, b:b + 1], axis=0, keepdims=True) for b in range(OWN)], axis=0)
    retained = jnp.sum(q * key, axis=1, keepdims=True) * value + decay * carried
    scaled = retained * lax.rsqrt(jnp.mean(retained * retained, axis=1, keepdims=True) + EPS)
    mall[k] = (out_gate / (1.0 + jnp.exp(-out_gate)) * scaled).astype(BF16)
    key_out[...] = key
    value_out[...] = value
    gather_y(1, mall)
    loads[11].wait()
    mixed = mall[...].astype(F32).reshape(R, DV).astype(BF16)
    product = jnp.dot(mixed, wm_v[...], preferred_element_type=F32)
    resid = (resid + scatter_x(1, product)).astype(BF16).astype(F32)

    out = half_mlp(2, resid, column(2), go_v, uo_v, do_v, (13, 14, 15))
    result[...] = out.T.astype(BF16)
    for kind in ("ax", "y", "ag", "rx"):
        flush(kind)


def on_device(tokens, gain_in, gate_in, up_in, down_in, gain_mix, w_query, w_key, w_value, w_gate,
              w_mixout, forget_rate, state_in, positions, gain_out, gate_out, up_out, down_out):
    NT = lax.axis_size("tp")
    NK = lax.axis_size("kv")
    NY = NK // 2
    R, c = tokens.shape
    C, FF = gate_in.shape
    OWN, _, DK, DV = state_in.shape
    D = C * NK
    mlp_pieces = widths(FF, (768,))
    qkv_pieces = [(0, 3 * DK)]
    dims = (NT, NY, NK, R, OWN, C, c, FF, DK, DV, D, mlp_pieces, qkv_pieces)

    def exchange(pieces, calls):
        wide = [last - first for first, last in pieces]
        return (
            [pltpu.VMEM((2, NY, 2 * OWN, w), BF16) for w in wide],
            [pltpu.VMEM((NY, 2 * OWN, w), BF16) for w in wide],
            [pltpu.VMEM((NY, 2 * OWN, w), BF16) for w in wide],
            [pltpu.VMEM((*calls, NY, 2 * OWN, w), BF16) for w in wide],
        )

    dma = pltpu.SemaphoreType.DMA
    n_p = len(mlp_pieces)
    scratch = [
        pltpu.VMEM((R, c), BF16), pltpu.VMEM((3, 1, c), BF16),
        pltpu.VMEM((C, FF), BF16), pltpu.VMEM((C, FF), BF16), pltpu.VMEM((FF, C), BF16),
        pltpu.VMEM((C, DK), BF16), pltpu.VMEM((C, DK), BF16), pltpu.VMEM((C, DV), BF16), pltpu.VMEM((C, DV), BF16),
        pltpu.VMEM((DV, C), BF16), pltpu.VMEM((OWN, DK, DV), F32),
        pltpu.VMEM((C, FF), BF16), pltpu.VMEM((C, FF), BF16), pltpu.VMEM((FF, C), BF16),
        dma((16,)),
        pltpu.VMEM((3, NT, c, R), BF16), pltpu.VMEM((3, 1, R), F32), pltpu.VMEM((3, NT, 1, R), F32),
        pltpu.VMEM((3, 1, R), F32), pltpu.VMEM((3, 1, R), F32), pltpu.VMEM((3, 1, R), F32),
        pltpu.VMEM((3, NY, 1, R), F32), pltpu.VMEM((3, R, 128), F32),
        *exchange(mlp_pieces, (2,)),
        *exchange(qkv_pieces, ()),
        pltpu.VMEM((2, NK, OWN, FF), BF16), pltpu.VMEM((NK, OWN, DV), BF16),
        pltpu.VMEM((3, NT, c, R), BF16), pltpu.VMEM((3, NT, c, R), BF16), pltpu.VMEM((c, R), F32),
        dma((NT,)), dma((NT,)), dma((n_p,)), dma((1,)), dma((n_p, NY)), dma((NY,)), dma((NY,)), dma((NY,)), dma((NT,)),
        dma((3, NT)), dma((3, NT)), dma((3, n_p)), dma((3,)), dma((3, n_p, NY)), dma((3, NY)), dma((3, NY)),
        dma((3, NY)), dma((3, NT)),
    ]
    smem = pl.BlockSpec(memory_space=pltpu.SMEM)
    hbm = pl.BlockSpec(memory_space=pl.ANY)
    vmem = pl.BlockSpec(memory_space=pltpu.VMEM)
    result, key, value = pl.pallas_call(
        functools.partial(kernel, dims),
        out_shape=(jax.ShapeDtypeStruct((R, c), BF16), jax.ShapeDtypeStruct((OWN, DK), F32),
                   jax.ShapeDtypeStruct((OWN, DV), F32)),
        in_specs=[hbm] * 4 + [smem] * 2 + [hbm] * 12,
        out_specs=(vmem, vmem, vmem),
        scratch_shapes=scratch,
        compiler_params=pltpu.CompilerParams(collective_id=0, has_side_effects=True,
                                             vmem_limit_bytes=40 * 1024 * 1024),
        name="layer_step",
    )(tokens, gain_in[None], gain_mix[None], gain_out[None], forget_rate, positions,
      gate_in, up_in, down_in, w_query, w_key, w_value, w_gate, w_mixout, state_in.reshape(OWN, DK, DV), gate_out, up_out, down_out)
    decay = jnp.exp(-forget_rate)
    new_state = decay[None, :, None, None] * state_in + key[:, None, :, None] * value[:, None, None, :]
    return result, new_state


KV_TP = ("kv", "tp")


def solution(mesh):
    feature, wide, tall = P(KV_TP), P("kv", "tp"), P("tp", "kv")
    state = P(("grp", "kv"), "tp", None, None)
    placed = (P("grp", KV_TP), feature, wide, wide, tall, feature, wide, wide, wide, wide, tall, P("tp"), state,
              P(("grp", "kv")), feature, wide, wide, tall)
    return jax.shard_map(on_device, mesh=mesh, in_specs=placed, out_specs=(P("grp", KV_TP), state), check_vma=False)
```

```python
import functools
import math

import jax
import jax.numpy as jnp
from jax import lax
from jax.experimental import pallas as pl
from jax.experimental.pallas import tpu as pltpu
from jax.sharding import PartitionSpec as P

EPS = 1e-06
BASE = 10000.0
MESH = pl.DeviceIdType.MESH
F32 = jnp.float32
BF16 = jnp.bfloat16


def far_first(n):
    return sorted(range(1, n), key=lambda j: -min(j, n - j))


def near_first(n):
    return sorted(range(1, n), key=lambda j: min(j, n - j))


def widths(total, cut):
    edges = [0, *[c for c in cut if c < total], total]
    return list(zip(edges[:-1], edges[1:]))


def tiles(first, last, step=256):
    return [(at, min(at + step, last)) for at in range(first, last, step)]


def kernel(dims, tokens, gain_in, gain_mix, gain_out, forget, positions,
           gate_in, up_in, down_in, w_query, w_key, w_value, w_gate, w_mix, state,
           gate_out, up_out, down_out,
           result, key_out, value_out, *scratch):
    NT, NY, NK, R, OWN, C, c, FF, DK, DV, D, mlp_pieces, qkv_pieces = dims
    (tok_v, gains_v, gi_v, ui_v, di_v, wq_v, wk_v, wv_v, wg_v, wm_v, st_v, go_v, uo_v, do_v, load_sem,
     xall, ss_src, ssx, ss_k, ss_b, ss_c, ssy, fac,
     part_m, sib_m, red_m, recv_m, part_q, sib_q, red_q, recv_q,
     hall, mall, px, rx, oT,
     ax_s, axs_s, sib_s, ssb_s, y_s, ssy_s, ag_s, agf_s, rx_s,
     ax_r, axs_r, sib_r, ssb_r, y_r, ssy_r, ag_r, agf_r, rx_r) = scratch

    t = lax.axis_index("tp")
    k = lax.axis_index("kv")
    core = lax.rem(k, 2)
    y = lax.div(k, 2)
    sibling = {"kv": k + 1 - 2 * core}

    def at_t(j):
        return lax.rem(t + j, NT)

    def at_y(j):
        return lax.rem(y + j, NY)

    def chip(j):
        return {"kv": 2 * at_y(j) + core}

    loads = []
    pairs = [(tokens, tok_v), (gain_in, gains_v.at[0]), (gain_mix, gains_v.at[1]), (gain_out, gains_v.at[2]),
             (gate_in, gi_v), (up_in, ui_v), (w_query, wq_v), (w_key, wk_v), (w_value, wv_v), (w_gate, wg_v),
             (down_in, di_v), (w_mix, wm_v), (state, st_v), (gate_out, go_v), (up_out, uo_v), (down_out, do_v)]
    for i, (src, dst) in enumerate(pairs):
        copy = pltpu.make_async_copy(src, dst, load_sem.at[i])
        copy.start()
        loads.append(copy)

    barrier = pltpu.get_barrier_semaphore()
    pl.semaphore_signal(barrier, inc=1, device_id=sibling, device_id_type=MESH)
    for j in far_first(NT):
        pl.semaphore_signal(barrier, inc=1, device_id={"tp": at_t(j)}, device_id_type=MESH)
    for j in far_first(NY):
        pl.semaphore_signal(barrier, inc=1, device_id=chip(j), device_id_type=MESH)

    for i in range(4):
        loads[i].wait()
    def column(i):
        row = jnp.broadcast_to(gains_v[i].astype(F32), (R, c))
        return row.T

    resid = tok_v[...].astype(F32)
    pl.semaphore_wait(barrier, 1 + (NT - 1) + (NY - 1))

    pending = {}

    def remote(src, dst, ssem, rsem, device):
        return pltpu.make_async_remote_copy(src_ref=src, dst_ref=dst, send_sem=ssem, recv_sem=rsem,
                                            device_id=device, device_id_type=MESH)

    def flush(kind):
        for copy in pending.pop(kind, []):
            copy.wait_send()

    def gather_x(s, normed, squares):
        flush("ax")
        xall[s, t] = normed
        ss_src[s] = squares
        copies, small = [], []
        for j in far_first(NT):
            copy = remote(xall.at[s, t], xall.at[s, t], ax_s.at[j], ax_r.at[s, NT - j], {"tp": at_t(j)})
            copy.start()
            copies.append(copy)
        for j in far_first(NT):
            copy = remote(ss_src.at[s], ssx.at[s, NT - j], axs_s.at[j], axs_r.at[s, NT - j], {"tp": at_t(j)})
            copy.start()
            small.append(copy)
        for j in near_first(NT):
            remote(xall.at[s, t], xall.at[s, t], ax_s.at[j], ax_r.at[s, j], {"tp": at_t(j)}).wait_recv()
        pending["ax"] = copies + small
        whole = xall[s].astype(F32).reshape(C, R)
        return whole.T.astype(BF16)

    def squares_of_block(s, own):
        total = own
        for j in near_first(NT):
            remote(ss_src.at[s], ssx.at[s, j], axs_s.at[j], axs_r.at[s, j], {"tp": at_t(j)}).wait_recv()
            total = total + ssx[s, j]
        return total

    def scatter_y(s, pieces, compute, part, sib, red, recv, own_squares, first_piece):
        flush("y")
        copies = []
        for p in range(len(pieces)):
            compute(p)
            copy = remote(part[p].at[1 - core], sib[p], sib_s.at[p], sib_r.at[s, p], sibling)
            copy.start()
            copies.append(copy)
        block = squares_of_block(s, own_squares)
        ss_k[s] = block
        copy = remote(ss_k.at[s], ss_b.at[s], ssb_s.at[0], ssb_r.at[s], sibling)
        copy.start()
        copies.append(copy)
        for p in range(len(pieces)):
            remote(part[p].at[1 - core], sib[p], sib_s.at[p], sib_r.at[s, p], sibling).wait_recv()
            late = None
            for j in far_first(NY) + [0]:
                yd = at_y(j)
                red[p][yd] = (part[p][core, yd].astype(F32) + sib[p][yd].astype(F32)).astype(BF16)
                if late is not None:
                    late.start()
                    copies.append(late)
                late = None
                if j:
                    late = remote(red[p].at[yd], recv[p].at[NY - j], y_s.at[p, j], y_r.at[s, p, NY - j], chip(j))
        remote(ss_k.at[s], ss_b.at[s], ssb_s.at[0], ssb_r.at[s], sibling).wait_recv()
        chip_sum = block + ss_b[s]
        ss_c[s] = chip_sum
        for j in far_first(NY):
            copy = remote(ss_c.at[s], ssy.at[s, NY - j], ssy_s.at[j], ssy_r.at[s, NY - j], chip(j))
            copy.start()
            copies.append(copy)
        pending["y"] = copies
        total = chip_sum
        for j in near_first(NY):
            remote(ss_c.at[s], ssy.at[s, j], ssy_s.at[j], ssy_r.at[s, j], chip(j)).wait_recv()
            total = total + ssy[s, j]
        wide = jnp.broadcast_to(total, (128, R)).T
        fac[s] = lax.rsqrt(wide / D + EPS)
        factor = fac[s, pl.ds(pl.multiple_of(k * OWN, OWN), OWN), :][:, :1]
        sums = []
        for p in range(len(pieces)):
            acc = red[p][y].astype(F32)
            for j in near_first(NY):
                remote(red[p].at[y], recv[p].at[j], y_s.at[p, j], y_r.at[s, p, j], chip(j)).wait_recv()
                acc = acc + recv[p][j].astype(F32)
            sums.append(acc)
        return sums, factor

    def gather_y(s, buf):
        flush("ag")
        copies = []
        copy = remote(buf.at[k], buf.at[k], agf_s.at[0], agf_r.at[s, 0], sibling)
        copy.start()
        copies.append(copy)
        for j in far_first(NY):
            copy = remote(buf.at[k], buf.at[k], ag_s.at[j], ag_r.at[s, NY - j], chip(j))
            copy.start()
            copies.append(copy)
        for j in near_first(NY):
            slot = 2 * at_y(j) + core
            remote(buf.at[slot], buf.at[slot], ag_s.at[j], ag_r.at[s, j], chip(j)).wait_recv()
            copy = remote(buf.at[slot], buf.at[slot], agf_s.at[j], agf_r.at[s, j], sibling)
            copy.start()
            copies.append(copy)
        for j in [0] + near_first(NY):
            slot = 2 * at_y(j) + 1 - core
            remote(buf.at[slot], buf.at[slot], agf_s.at[j], agf_r.at[s, j], sibling).wait_recv()
        pending["ag"] = copies

    def scatter_x(s, product):
        flush("rx")
        px[s] = product.T.reshape(NT, c, R).astype(BF16)
        copies = []
        for j in far_first(NT):
            copy = remote(px.at[s, at_t(j)], rx.at[s, NT - j], rx_s.at[j], rx_r.at[s, NT - j], {"tp": at_t(j)})
            copy.start()
            copies.append(copy)
        pending["rx"] = copies
        total = px[s, t].astype(F32)
        for j in near_first(NT):
            remote(px.at[s, at_t(j)], rx.at[s, j], rx_s.at[j], rx_r.at[s, j], {"tp": at_t(j)}).wait_recv()
            total = total + rx[s, j].astype(F32)
        return total

    def half_mlp(s, resid, gain, gate, up, down, waits):
        squares = jnp.sum(resid * resid, axis=0, keepdims=True)
        normed = gather_x(s, (resid * gain).astype(BF16), squares)
        for i in waits[:2]:
            loads[i].wait()

        def compute(p):
            first, last = mlp_pieces[p]
            for lo, hi in tiles(first, last):
                g = lax.dot_general(normed, gate[lo:hi], (((1,), (1,)), ((), ())), preferred_element_type=F32)
                u = lax.dot_general(normed, up[lo:hi], (((1,), (1,)), ((), ())), preferred_element_type=F32)
                for kk in range(NK):
                    rows = slice(OWN * kk, OWN * kk + OWN)
                    part_m[p][kk % 2, kk // 2, :, lo - first:hi - first] = jnp.concatenate(
                        [g[rows], u[rows]], axis=0).astype(BF16)

        sums, factor = scatter_y(s, mlp_pieces, compute, part_m, sib_m, red_m, [r.at[s // 2] for r in recv_m],
                                 squares, 0)
        for (first, last), acc in zip(mlp_pieces, sums):
            g = factor * acc[:OWN]
            u = factor * acc[OWN:]
            hall[s // 2, k, :, first:last] = (g / (1.0 + jnp.exp(-g)) * u).astype(BF16)
        gather_y(s, hall.at[s // 2])
        loads[waits[2]].wait()
        hidden = hall[s // 2].astype(F32).reshape(R, FF).astype(BF16)
        product = jnp.dot(hidden, down[...], preferred_element_type=F32)
        return resid + 0.5 * scatter_x(s, product)

    resid = half_mlp(0, resid, column(0), gi_v, ui_v, di_v, (4, 5, 10)).astype(BF16).astype(F32)

    squares = jnp.sum(resid * resid, axis=0, keepdims=True)
    normed = gather_x(1, (resid * column(1)).astype(BF16), squares)
    for i in (6, 7, 8, 9):
        loads[i].wait()

    def compute_qkv(p):
        q = jnp.dot(normed, wq_v[...], preferred_element_type=F32)
        kk_ = jnp.dot(normed, wk_v[...], preferred_element_type=F32)
        v = jnp.dot(normed, wv_v[...], preferred_element_type=F32)
        g = jnp.dot(normed, wg_v[...], preferred_element_type=F32)
        half = DV // 2
        top = [q, kk_, v[:, :half]]
        low = [v[:, half:], g[:, :half], g[:, half:]]
        for i in range(3):
            for kk in range(NK):
                rows = slice(OWN * kk, OWN * kk + OWN)
                part_q[0][kk % 2, kk // 2, :, DK * i:DK * i + DK] = jnp.concatenate(
                    [top[i][rows], low[i][rows]], axis=0).astype(BF16)

    sums, factor = scatter_y(1, qkv_pieces, compute_qkv, part_q, sib_q, red_q, recv_q, squares, 0)
    acc = (jnp.concatenate([factor, factor], axis=0) * sums[0]).astype(BF16).astype(F32)
    q, key = acc[:OWN, :DK], acc[:OWN, DK:2 * DK]
    value = jnp.concatenate([acc[:OWN, 2 * DK:], acc[OWN:, :DK]], axis=1)
    out_gate = acc[OWN:, DK:]

    row = lax.broadcasted_iota(jnp.int32, (OWN, DK), 0)
    lane = lax.broadcasted_iota(jnp.int32, (OWN, DK), 1)
    place = jnp.zeros((OWN, DK), F32)
    for r in range(OWN):
        place = jnp.where(row == r, positions[r].astype(F32), place)
    half = DK // 2
    pair = jnp.where(lane < half, lane, lane - half).astype(F32)
    angle = place * jnp.exp(pair * (-2.0 * math.log(BASE) / DK))
    cosine = jnp.cos(angle)
    sine = jnp.where(lane < half, -jnp.sin(angle), jnp.sin(angle))

    def rotate(v):
        return v * cosine + jnp.concatenate([v[:, half:], v[:, :half]], axis=1) * sine

    q = rotate(q)
    key = rotate(key) * DK ** (-0.5)
    decay = jnp.exp(jnp.broadcast_to(-forget[0], (1, DV)))
    q_col = q.T
    loads[12].wait()
    carried = jnp.concatenate(
        [jnp.sum(st_v[b] * q_col[:, b:b + 1], axis=0, keepdims=True) for b in range(OWN)], axis=0)
    retained = jnp.sum(q * key, axis=1, keepdims=True) * value + decay * carried
    scaled = retained * lax.rsqrt(jnp.mean(retained * retained, axis=1, keepdims=True) + EPS)
    mall[k] = (out_gate / (1.0 + jnp.exp(-out_gate)) * scaled).astype(BF16)
    key_out[...] = key
    value_out[...] = value
    gather_y(1, mall)
    loads[11].wait()
    mixed = mall[...].astype(F32).reshape(R, DV).astype(BF16)
    product = jnp.dot(mixed, wm_v[...], preferred_element_type=F32)
    resid = (resid + scatter_x(1, product)).astype(BF16).astype(F32)

    out = half_mlp(2, resid, column(2), go_v, uo_v, do_v, (13, 14, 15))
    result[...] = out.astype(BF16)
    for kind in ("ax", "y", "ag", "rx"):
        flush(kind)


def on_device(tokens, gain_in, gate_in, up_in, down_in, gain_mix, w_query, w_key, w_value, w_gate,
              w_mixout, forget_rate, state_in, positions, gain_out, gate_out, up_out, down_out):
    NT = lax.axis_size("tp")
    NK = lax.axis_size("kv")
    NY = NK // 2
    R, c = tokens.shape
    C, FF = gate_in.shape
    OWN, _, DK, DV = state_in.shape
    D = C * NK
    mlp_pieces = widths(FF, (768,))
    qkv_pieces = [(0, 3 * DK)]
    dims = (NT, NY, NK, R, OWN, C, c, FF, DK, DV, D, mlp_pieces, qkv_pieces)

    def exchange(pieces, calls):
        wide = [last - first for first, last in pieces]
        return (
            [pltpu.VMEM((2, NY, 2 * OWN, w), BF16) for w in wide],
            [pltpu.VMEM((NY, 2 * OWN, w), BF16) for w in wide],
            [pltpu.VMEM((NY, 2 * OWN, w), BF16) for w in wide],
            [pltpu.VMEM((*calls, NY, 2 * OWN, w), BF16) for w in wide],
        )

    dma = pltpu.SemaphoreType.DMA
    n_p = len(mlp_pieces)
    scratch = [
        pltpu.VMEM((c, R), BF16), pltpu.VMEM((3, 1, c), BF16),
        pltpu.VMEM((FF, C), BF16), pltpu.VMEM((FF, C), BF16), pltpu.VMEM((FF, C), BF16),
        pltpu.VMEM((C, DK), BF16), pltpu.VMEM((C, DK), BF16), pltpu.VMEM((C, DV), BF16), pltpu.VMEM((C, DV), BF16),
        pltpu.VMEM((DV, C), BF16), pltpu.VMEM((OWN, DK, DV), F32),
        pltpu.VMEM((FF, C), BF16), pltpu.VMEM((FF, C), BF16), pltpu.VMEM((FF, C), BF16),
        dma((16,)),
        pltpu.VMEM((3, NT, c, R), BF16), pltpu.VMEM((3, 1, R), F32), pltpu.VMEM((3, NT, 1, R), F32),
        pltpu.VMEM((3, 1, R), F32), pltpu.VMEM((3, 1, R), F32), pltpu.VMEM((3, 1, R), F32),
        pltpu.VMEM((3, NY, 1, R), F32), pltpu.VMEM((3, R, 128), F32),
        *exchange(mlp_pieces, (2,)),
        *exchange(qkv_pieces, ()),
        pltpu.VMEM((2, NK, OWN, FF), BF16), pltpu.VMEM((NK, OWN, DV), BF16),
        pltpu.VMEM((3, NT, c, R), BF16), pltpu.VMEM((3, NT, c, R), BF16), pltpu.VMEM((c, R), F32),
        dma((NT,)), dma((NT,)), dma((n_p,)), dma((1,)), dma((n_p, NY)), dma((NY,)), dma((NY,)), dma((NY,)), dma((NT,)),
        dma((3, NT)), dma((3, NT)), dma((3, n_p)), dma((3,)), dma((3, n_p, NY)), dma((3, NY)), dma((3, NY)),
        dma((3, NY)), dma((3, NT)),
    ]
    smem = pl.BlockSpec(memory_space=pltpu.SMEM)
    hbm = pl.BlockSpec(memory_space=pl.ANY)
    vmem = pl.BlockSpec(memory_space=pltpu.VMEM)
    result, key, value = pl.pallas_call(
        functools.partial(kernel, dims),
        out_shape=(jax.ShapeDtypeStruct((c, R), BF16), jax.ShapeDtypeStruct((OWN, DK), F32),
                   jax.ShapeDtypeStruct((OWN, DV), F32)),
        in_specs=[hbm] * 4 + [smem] * 2 + [hbm] * 12,
        out_specs=(vmem, vmem, vmem),
        scratch_shapes=scratch,
        compiler_params=pltpu.CompilerParams(collective_id=0, has_side_effects=True,
                                             vmem_limit_bytes=67043328),
        name="layer_step",
    )(tokens.T, gain_in[None], gain_mix[None], gain_out[None], forget_rate, positions,
      gate_in.T, up_in.T, down_in, w_query, w_key, w_value, w_gate, w_mixout, state_in.reshape(OWN, DK, DV),
      gate_out.T, up_out.T, down_out)
    decay = jnp.exp(-forget_rate)
    new_state = decay[None, :, None, None] * state_in + key[:, None, :, None] * value[:, None, None, :]
    return result.T, new_state


KV_TP = ("kv", "tp")


def solution(mesh):
    feature, wide, tall = P(KV_TP), P("kv", "tp"), P("tp", "kv")
    state = P(("grp", "kv"), "tp", None, None)
    placed = (P("grp", KV_TP), feature, wide, wide, tall, feature, wide, wide, wide, wide, tall, P("tp"), state,
              P(("grp", "kv")), feature, wide, wide, tall)
    return jax.shard_map(on_device, mesh=mesh, in_specs=placed, out_specs=(P("grp", KV_TP), state), check_vma=False)
```

```python
import functools
import math

import jax
import jax.numpy as jnp
from jax import lax
from jax.experimental import pallas as pl
from jax.experimental.pallas import tpu as pltpu
from jax.sharding import PartitionSpec as P

EPS = 1e-06
BASE = 10000.0
MESH = pl.DeviceIdType.MESH
F32 = jnp.float32
BF16 = jnp.bfloat16


def far_first(n):
    return sorted(range(1, n), key=lambda j: -min(j, n - j))


def near_first(n):
    return sorted(range(1, n), key=lambda j: min(j, n - j))


def widths(total, cut):
    edges = [0, *[c for c in cut if c < total], total]
    return list(zip(edges[:-1], edges[1:]))


def tiles(first, last, step=256):
    return [(at, min(at + step, last)) for at in range(first, last, step)]


def kernel(dims, tokens, gain_in, gain_mix, gain_out, forget, positions,
           gate_in, up_in, down_in, w_query, w_key, w_value, w_gate, w_mix, state,
           gate_out, up_out, down_out,
           result, state_out, *scratch):
    NT, NY, NK, R, OWN, C, c, FF, FP, DK, DV, D, mlp_pieces, qkv_pieces = dims
    (tok_v, gains_v, gi_v, ui_v, di_v, wq_v, wk_v, wv_v, wg_v, wm_v, st_v, go_v, uo_v, do_v, rate_v, place_v, next_v, load_sem,
     xall, ss_src, ssx, ss_k, ss_b, ss_c, ssy, fac,
     part_m, sib_m, red_m, recv_m, part_q, sib_q, red_q, recv_q,
     hall, mall, rows_v, px, rx,
     ax_s, axs_s, sib_s, ssb_s, y_s, ssy_s, ag_s, agf_s, rx_s,
     ax_r, axs_r, sib_r, ssb_r, y_r, ssy_r, ag_r, agf_r, rx_r) = scratch

    t = lax.axis_index("tp")
    k = lax.axis_index("kv")
    core = lax.rem(k, 2)
    y = lax.div(k, 2)
    sibling = {"kv": k + 1 - 2 * core}
    HALF = NY // 2

    def at_t(j):
        return lax.rem(t + j, NT)

    def at_y(j):
        return lax.rem(y + j, NY)

    def chip(j):
        return {"kv": 2 * at_y(j) + core}

    barrier = pltpu.get_barrier_semaphore()
    for j in far_first(NT):
        pl.semaphore_signal(barrier, inc=1, device_id={"tp": at_t(j)}, device_id_type=MESH)
    for j in far_first(NY):
        pl.semaphore_signal(barrier, inc=1, device_id=chip(j), device_id_type=MESH)
    pl.semaphore_signal(barrier, inc=1, device_id=sibling, device_id_type=MESH)

    loads = []
    pairs = [(tokens, tok_v), (gain_in, gains_v.at[0]), (gain_mix, gains_v.at[1]), (gain_out, gains_v.at[2]),
             (gate_in, gi_v), (up_in, ui_v), (w_query, wq_v), (w_key, wk_v), (w_value, wv_v), (w_gate, wg_v),
             (down_in, di_v), (w_mix, wm_v), (state, st_v), (gate_out, go_v), (up_out, uo_v), (down_out, do_v),
             (forget, rate_v), (positions, place_v)]
    for i, (src, dst) in enumerate(pairs):
        if src.shape[0] < dst.shape[0]:
            dst = dst.at[pl.ds(0, src.shape[0])]
        copy = pltpu.make_async_copy(src, dst, load_sem.at[i])
        copy.start()
        loads.append(copy)
    if FP > FF:
        for full in (gi_v, ui_v, di_v, go_v, uo_v, do_v):
            full[FF:] = jnp.zeros((FP - FF, C), BF16)
    for i in range(4):
        loads[i].wait()

    def column(i):
        row = jnp.broadcast_to(gains_v[i].astype(F32), (R, c))
        return row.T

    resid = tok_v[...].astype(F32)
    pl.semaphore_wait(barrier, 1 + (NT - 1) + (NY - 1))

    pending = {}

    def remote(src, dst, ssem, rsem, device):
        return pltpu.make_async_remote_copy(src_ref=src, dst_ref=dst, send_sem=ssem, recv_sem=rsem,
                                            device_id=device, device_id_type=MESH)

    def send(kind, copy):
        copy.start()
        pending.setdefault(kind, []).append(copy)

    def flush(kind):
        for copy in pending.pop(kind, []):
            copy.wait_send()

    @jax.named_scope("gather_x")
    def gather_x(s, normed, squares):
        flush("ax")
        xall[s, t] = normed
        ss_src[s] = squares
        for j in far_first(NT):
            send("ax", remote(xall.at[s, t], xall.at[s, t], ax_s.at[j], ax_r.at[s, NT - j], {"tp": at_t(j)}))
        for j in far_first(NT):
            send("ax", remote(ss_src.at[s], ssx.at[s, NT - j], axs_s.at[j], axs_r.at[s, NT - j], {"tp": at_t(j)}))
        for j in near_first(NT):
            remote(xall.at[s, t], xall.at[s, t], ax_s.at[j], ax_r.at[s, j], {"tp": at_t(j)}).wait_recv()
        whole = xall[s].astype(F32).reshape(C, R)
        return whole.T.astype(BF16)

    class Reduce:
        def __init__(self, s, part, sib, red, recv, relay, squares):
            self.s, self.part, self.sib, self.red, self.recv = s, part, sib, red, recv
            self.relay, self.squares = relay, squares
            flush("y")

        def side(self, p):
            return 1 if p % 2 == 0 else NY - 1

        def swap(self, p):
            return remote(self.part[p].at[1 - core], self.sib[p], sib_s.at[p], sib_r.at[self.s, p], sibling)

        def hop(self, p, j, device_j, slot):
            return remote(self.red[p].at[at_y(j)], self.recv[p].at[slot], y_s.at[p, j], y_r.at[self.s, p, slot],
                          chip(device_j))

        def arrived(self, p, slot):
            self.hop(p, slot, slot, slot).wait_recv()
            return self.recv[p][slot].astype(F32)

        def both(self, p, yd):
            return self.part[p][core, yd].astype(F32) + self.sib[p][yd].astype(F32)

        def start_squares(self):
            s, block = self.s, self.squares
            for j in near_first(NT):
                remote(ss_src.at[s], ssx.at[s, j], axs_s.at[j], axs_r.at[s, j], {"tp": at_t(j)}).wait_recv()
                block = block + ssx[s, j]
            ss_k[s] = block
            self.block = block
            send("y", remote(ss_k.at[s], ss_b.at[s], ssb_s.at[0], ssb_r.at[s], sibling))

        def send_squares(self):
            s = self.s
            remote(ss_k.at[s], ss_b.at[s], ssb_s.at[0], ssb_r.at[s], sibling).wait_recv()
            self.block = self.block + ss_b[s]
            ss_c[s] = self.block
            for j in far_first(NY):
                send("y", remote(ss_c.at[s], ssy.at[s, NY - j], ssy_s.at[j], ssy_r.at[s, NY - j], chip(j)))

        def factor(self):
            s, total = self.s, self.block
            for j in near_first(NY):
                remote(ss_c.at[s], ssy.at[s, j], ssy_s.at[j], ssy_r.at[s, j], chip(j)).wait_recv()
                total = total + ssy[s, j]
            fac[s] = lax.rsqrt(jnp.broadcast_to(total, (128, R)).T / D + EPS)
            return fac[s, pl.ds(pl.multiple_of(k * OWN, OWN), OWN), :][:, :1]

        @jax.named_scope("send_piece")
        def send_piece(self, p):
            self.swap(p).wait_recv()
            side = self.side(p)
            late = None
            for j in far_first(NY):
                last = HALF - 1 if side == 1 else HALF + 1
                if self.relay and j == last:
                    continue
                yd = at_y(j)
                self.red[p][yd] = self.both(p, yd).astype(BF16)
                if late is not None:
                    send("y", late)
                if self.relay and j == HALF:
                    late = self.hop(p, j, side, HALF)
                else:
                    late = self.hop(p, j, j, NY - j)
            send("y", late)

        @jax.named_scope("send_relayed")
        def send_relayed(self, p):
            if not self.relay:
                return
            last = HALF - 1 if self.side(p) == 1 else HALF + 1
            yd = at_y(last)
            self.red[p][yd] = (self.both(p, yd) + self.arrived(p, HALF)).astype(BF16)
            send("y", self.hop(p, last, last, NY - last))

        @jax.named_scope("collect")
        def collect(self, p):
            acc = self.both(p, y)
            for j in near_first(NY):
                if not (self.relay and j == HALF):
                    acc = acc + self.arrived(p, j)
            return acc

    class Gather:
        def __init__(self, s, bufs, relay):
            self.s, self.bufs, self.relay = s, bufs, relay
            flush("ag")

        def same(self, p, slot, j, device_j, off):
            ref = self.bufs[p].at[slot]
            return remote(ref, ref, ag_s.at[p, j], ag_r.at[self.s, p, off], chip(device_j))

        def over(self, p, slot, off):
            ref = self.bufs[p].at[slot]
            return remote(ref, ref, agf_s.at[p, off], agf_r.at[self.s, p, off], sibling)

        def start(self, p):
            for j in far_first(NY):
                if not (self.relay and j == HALF):
                    send("ag", self.same(p, k, j, j, NY - j))
            send("ag", self.over(p, k, 0))

        @jax.named_scope("forward")
        def forward(self, p):
            side = 1 if p % 2 == 0 else NY - 1
            source = HALF + 1 if side == 1 else HALF - 1
            order = [j for j in near_first(NY) if j != HALF]
            order.sort(key=lambda j: (min(j, NY - j), j != source))
            for j in order + [HALF]:
                slot = 2 * at_y(j) + core
                self.same(p, slot, j, j, j).wait_recv()
                if self.relay and j == source:
                    send("ag", self.same(p, slot, HALF, side, HALF))
                send("ag", self.over(p, slot, j))

        @jax.named_scope("finish")
        def finish(self, p, rows, first, last):
            for j in [0] + near_first(NY):
                yd = at_y(j)
                self.over(p, 2 * yd + 1 - core, j).wait_recv()
                pair = jnp.concatenate([self.bufs[p][2 * yd].astype(F32), self.bufs[p][2 * yd + 1].astype(F32)], axis=0)
                rows[pl.ds(pl.multiple_of(2 * OWN * yd, 2 * OWN), 2 * OWN), first:last] = pair.astype(BF16)

    @jax.named_scope("scatter_x")
    def scatter_x(s, product):
        flush("rx")
        px[s] = product.T.reshape(NT, c, R).astype(BF16)
        for j in far_first(NT):
            send("rx", remote(px.at[s, at_t(j)], rx.at[s, NT - j], rx_s.at[j], rx_r.at[s, NT - j], {"tp": at_t(j)}))
        total = px[s, t].astype(F32)
        for j in near_first(NT):
            remote(px.at[s, at_t(j)], rx.at[s, j], rx_s.at[j], rx_r.at[s, j], {"tp": at_t(j)}).wait_recv()
            total = total + rx[s, j].astype(F32)
        return total

    def half_mlp(s, resid, gain, gate, up, down, waits):
        m = s // 2
        count = len(mlp_pieces)
        squares = jnp.sum(resid * resid, axis=0, keepdims=True)
        normed = gather_x(s, (resid * gain).astype(BF16), squares)
        for i in waits[:2]:
            loads[i].wait()
        reduce = Reduce(s, part_m, sib_m, red_m, [r.at[m] for r in recv_m], False, squares)
        for p, (first, last) in enumerate(mlp_pieces):
            with jax.named_scope("mm_up"):
                for lo, hi in tiles(first, last):
                    g = lax.dot_general(normed, gate[lo:hi], (((1,), (1,)), ((), ())), preferred_element_type=F32)
                    u = lax.dot_general(normed, up[lo:hi], (((1,), (1,)), ((), ())), preferred_element_type=F32)
                    for kk in range(NK):
                        rows = slice(OWN * kk, OWN * kk + OWN)
                        part_m[p][kk % 2, kk // 2, :, lo - first:hi - first] = jnp.concatenate(
                            [g[rows], u[rows]], axis=0).astype(BF16)
            send("y", reduce.swap(p))
            if p == 0:
                reduce.start_squares()
        reduce.send_squares()
        for p in range(count):
            reduce.send_piece(p)
            if p:
                reduce.send_relayed(p - 1)
        reduce.send_relayed(count - 1)
        factor = reduce.factor()
        gather = Gather(s, [h.at[m] for h in hall], False)
        for p in range(count):
            acc = reduce.collect(p)
            g = factor * acc[:OWN]
            u = factor * acc[OWN:]
            hall[p][m, k] = (g / (1.0 + jnp.exp(-g)) * u).astype(BF16)
            gather.start(p)
        loads[waits[2]].wait()
        product = None
        for p in range(count + 1):
            if p < count:
                gather.forward(p)
            if p:
                first, last = mlp_pieces[p - 1]
                gather.finish(p - 1, rows_v, first, last)
                term = jnp.dot(rows_v[:, first:last], down[first:last], preferred_element_type=F32)
                product = term if product is None else product + term
        return resid + 0.5 * scatter_x(s, product)

    resid = half_mlp(0, resid, column(0), gi_v, ui_v, di_v, (4, 5, 10)).astype(BF16).astype(F32)

    squares = jnp.sum(resid * resid, axis=0, keepdims=True)
    normed = gather_x(1, (resid * column(1)).astype(BF16), squares)
    for i in (6, 7, 8, 9, 16, 17):
        loads[i].wait()
    reduce = Reduce(1, part_q, sib_q, red_q, recv_q, False, squares)
    q = jnp.dot(normed, wq_v[...], preferred_element_type=F32)
    key = jnp.dot(normed, wk_v[...], preferred_element_type=F32)
    value = jnp.dot(normed, wv_v[...], preferred_element_type=F32)
    out_gate = jnp.dot(normed, wg_v[...], preferred_element_type=F32)
    half = DV // 2
    top = [q, key, value[:, :half]]
    low = [value[:, half:], out_gate[:, :half], out_gate[:, half:]]
    for i in range(3):
        for kk in range(NK):
            rows = slice(OWN * kk, OWN * kk + OWN)
            part_q[0][kk % 2, kk // 2, :, DK * i:DK * i + DK] = jnp.concatenate(
                [top[i][rows], low[i][rows]], axis=0).astype(BF16)
    send("y", reduce.swap(0))
    reduce.start_squares()
    reduce.send_squares()
    reduce.send_piece(0)

    row = lax.broadcasted_iota(jnp.int32, (OWN, DK), 0)
    lane = lax.broadcasted_iota(jnp.int32, (OWN, DK), 1)
    place = jnp.zeros((OWN, DK), F32)
    for r in range(OWN):
        place = jnp.where(row == r, place_v[r].astype(F32), place)
    half = DK // 2
    pair = jnp.where(lane < half, lane, lane - half).astype(F32)
    angle = place * jnp.exp(pair * (-2.0 * math.log(BASE) / DK))
    cosine = jnp.cos(angle)
    sine = jnp.where(lane < half, -jnp.sin(angle), jnp.sin(angle))
    decay = jnp.exp(-jnp.broadcast_to(rate_v[...], (1, DV)))
    loads[12].wait()

    factor = reduce.factor()
    acc = reduce.collect(0)
    acc = (jnp.concatenate([factor, factor], axis=0) * acc).astype(BF16).astype(F32)
    q, key = acc[:OWN, :DK], acc[:OWN, DK:2 * DK]
    value = jnp.concatenate([acc[:OWN, 2 * DK:], acc[OWN:, :DK]], axis=1)
    out_gate = acc[OWN:, DK:]

    def rotate(v):
        return v * cosine + jnp.concatenate([v[:, half:], v[:, :half]], axis=1) * sine

    with jax.named_scope("retain"):
        q = rotate(q)
        key = rotate(key) * DK ** (-0.5)
        q_col = q.T
        carried = jnp.concatenate(
            [jnp.sum(st_v[b] * q_col[:, b:b + 1], axis=0, keepdims=True) for b in range(OWN)], axis=0)
        retained = jnp.sum(q * key, axis=1, keepdims=True) * value + decay * carried
        scaled = retained * lax.rsqrt(jnp.mean(retained * retained, axis=1, keepdims=True) + EPS)
        gather = Gather(1, [mall], False)
        mall[k] = (out_gate / (1.0 + jnp.exp(-out_gate)) * scaled).astype(BF16)
        gather.start(0)
    with jax.named_scope("new_state"):
        key_col = key.T
        for b in range(OWN):
            next_v[b] = decay * st_v[b] + key_col[:, b:b + 1] * value[b:b + 1, :]
        keep = pltpu.make_async_copy(next_v, state_out, load_sem.at[18])
        keep.start()
    loads[11].wait()
    gather.forward(0)
    gather.finish(0, rows_v, 0, DV)
    product = jnp.dot(rows_v[:, :DV], wm_v[...], preferred_element_type=F32)
    resid = (resid + scatter_x(1, product)).astype(BF16).astype(F32)

    out = half_mlp(2, resid, column(2), go_v, uo_v, do_v, (13, 14, 15))
    result[...] = out.astype(BF16)
    keep.wait()
    for kind in ("ax", "y", "ag", "rx"):
        flush(kind)


def on_device(tokens, gain_in, gate_in, up_in, down_in, gain_mix, w_query, w_key, w_value, w_gate,
              w_mixout, forget_rate, state_in, positions, gain_out, gate_out, up_out, down_out):
    NT = lax.axis_size("tp")
    NK = lax.axis_size("kv")
    NY = NK // 2
    R, c = tokens.shape
    C, FF = gate_in.shape
    OWN, _, DK, DV = state_in.shape
    D = C * NK
    FP = -(-FF // 128) * 128
    mlp_pieces = widths(FP, (768,))
    qkv_pieces = [(0, 3 * DK)]
    dims = (NT, NY, NK, R, OWN, C, c, FF, FP, DK, DV, D, mlp_pieces, qkv_pieces)

    def exchange(pieces, calls):
        wide = [last - first for first, last in pieces]
        return (
            [pltpu.VMEM((2, NY, 2 * OWN, w), BF16) for w in wide],
            [pltpu.VMEM((NY, 2 * OWN, w), BF16) for w in wide],
            [pltpu.VMEM((NY, 2 * OWN, w), BF16) for w in wide],
            [pltpu.VMEM((*calls, NY, 2 * OWN, w), BF16) for w in wide],
        )

    dma = pltpu.SemaphoreType.DMA
    n_p = len(mlp_pieces)
    scratch = [
        pltpu.VMEM((c, R), BF16), pltpu.VMEM((3, 1, c), BF16),
        pltpu.VMEM((FP, C), BF16), pltpu.VMEM((FP, C), BF16), pltpu.VMEM((FP, C), BF16),
        pltpu.VMEM((C, DK), BF16), pltpu.VMEM((C, DK), BF16), pltpu.VMEM((C, DV), BF16), pltpu.VMEM((C, DV), BF16),
        pltpu.VMEM((DV, C), BF16), pltpu.VMEM((OWN, DK, DV), F32),
        pltpu.VMEM((FP, C), BF16), pltpu.VMEM((FP, C), BF16), pltpu.VMEM((FP, C), BF16),
        pltpu.VMEM((1, 1), F32), pltpu.SMEM((OWN,), jnp.int32), pltpu.VMEM((OWN, DK, DV), F32), dma((19,)),
        pltpu.VMEM((3, NT, c, R), BF16), pltpu.VMEM((3, 1, R), F32), pltpu.VMEM((3, NT, 1, R), F32),
        pltpu.VMEM((3, 1, R), F32), pltpu.VMEM((3, 1, R), F32), pltpu.VMEM((3, 1, R), F32),
        pltpu.VMEM((3, NY, 1, R), F32), pltpu.VMEM((3, R, 128), F32),
        *exchange(mlp_pieces, (2,)),
        *exchange(qkv_pieces, ()),
        [pltpu.VMEM((2, NK, OWN, b - a), BF16) for a, b in mlp_pieces], pltpu.VMEM((NK, OWN, DV), BF16),
        pltpu.VMEM((R, FP), BF16),
        pltpu.VMEM((3, NT, c, R), BF16), pltpu.VMEM((3, NT, c, R), BF16),
        dma((NT,)), dma((NT,)), dma((n_p,)), dma((1,)), dma((n_p, NY)), dma((NY,)), dma((n_p, NY)), dma((n_p, NY)),
        dma((NT,)),
        dma((3, NT)), dma((3, NT)), dma((3, n_p)), dma((3,)), dma((3, n_p, NY)), dma((3, NY)), dma((3, n_p, NY)),
        dma((3, n_p, NY)), dma((3, NT)),
    ]
    hbm = pl.BlockSpec(memory_space=pltpu.HBM)
    vmem = pl.BlockSpec(memory_space=pltpu.VMEM)
    result, new_state = pl.pallas_call(
        functools.partial(kernel, dims),
        out_shape=(jax.ShapeDtypeStruct((c, R), BF16), jax.ShapeDtypeStruct((OWN, DK, DV), F32)),
        in_specs=[hbm] * 18,
        out_specs=(vmem, hbm),
        scratch_shapes=scratch,
        compiler_params=pltpu.CompilerParams(collective_id=0, has_side_effects=True,
                                             vmem_limit_bytes=67043328),
        name="layer_step",
    )(tokens.T, gain_in[None], gain_mix[None], gain_out[None], forget_rate[None], positions,
      gate_in.T, up_in.T, down_in, w_query, w_key, w_value, w_gate, w_mixout, state_in.reshape(OWN, DK, DV),
      gate_out.T, up_out.T, down_out)
    return result.T, new_state.reshape(state_in.shape)


KV_TP = ("kv", "tp")


def solution(mesh):
    feature, wide, tall = P(KV_TP), P("kv", "tp"), P("tp", "kv")
    state = P(("grp", "kv"), "tp", None, None)
    placed = (P("grp", KV_TP), feature, wide, wide, tall, feature, wide, wide, wide, wide, tall, P("tp"), state,
              P(("grp", "kv")), feature, wide, wide, tall)
    return jax.shard_map(on_device, mesh=mesh, in_specs=placed, out_specs=(P("grp", KV_TP), state), check_vma=False)
```
